256 devices in a mesh: ep: 64 (over z, y, core), tp: 4 (over x).
Axes of the slice: x: 4, y: 4, z: 8, core: 2. Of those that a mesh axis runs over, the one named last changes fastest.
Arguments:
- mix_input: bfloat16 [65536, 2048], P(('ep', 'tp')), may hold values from -6 to 6
- mix_gain: float32 [2048], replicated, may hold values from 0.1 to 1.9
- pool_weight: bfloat16 [4, 512, 512], replicated, may hold values from -0.25 to 0.25
- pool_scale: float32 [2048], replicated, may hold values from 0.1 to 1.9
- moe_input: bfloat16 [32768, 2048], P(('ep', 'tp')), may hold values from -6 to 6
- moe_gain: float32 [2048], replicated, may hold values from 0.1 to 1.9
- expert_ids: int32 [32768, 4], P('ep'), may hold values from 0 to 127, all different within a row; in each aligned block of 128 rows (0 to 127, 128 to 255, ...) at most 6 rows name the same one
- route_score: float32 [32768, 4], P(('ep', 'tp')), may hold values from 0.05 to 1
- expert_gate: bfloat16 [128, 2048, 1024], P('ep', None, 'tp'), may hold values from -0.125 to 0.125
- expert_up: bfloat16 [128, 2048, 1024], P('ep', None, 'tp'), may hold values from -0.125 to 0.125
- expert_down: bfloat16 [128, 1024, 2048], P('ep', 'tp'), may hold values from -0.1875 to 0.1875
- shared_gate: bfloat16 [2048, 512], P(None, 'tp'), may hold values from -0.125 to 0.125
- shared_up: bfloat16 [2048, 512], P(None, 'tp'), may hold values from -0.125 to 0.125
- shared_down: bfloat16 [512, 2048], P('tp'), may hold values from -0.25 to 0.25
Outputs:
- mix_output: bfloat16 [65536, 2048], P(('ep', 'tp'))
- moe_output: bfloat16 [32768, 2048], P(('ep', 'tp'))
The draws below stay inside these ranges and needn't reach their ends.
Inputs may be any that keep to these rules, and one draw needn't show every extreme that they name: `expert_ids`: each row names 4 different experts. Within each aligned block of 128 rows (the tokens of one device) no expert is named by more than 6 rows, a bound that some block reaches.
All inputs are finite; a program needn't handle non-finite values.
Results may differ from the reference program's by a relative error of at most 0.012.
Values may be sent and summed in bfloat16 or wider, within the bound.
No kernel may reach another device: no remote copies, remote signals or barrier semaphores. Data moves between devices by JAX's collectives and lax.ppermute only.
A program may use at most 192 MiB of HBM per device.

```python
import math
import jax
import jax.numpy as jnp
import numpy as np
from jax import lax

D = 2048
GROUP = 512
FF = 1024
SH = 512
EXPERTS = 128
TOPK = 4
TOK_B = 128
TOKENS_A = 65536
TOKENS_B = 32768
CAP = 6
N_TP = 4


def levels(own_key, dims, shards, least, high):
    factor_of = 1.0
    for dim, blocks in shards:
        draws = jax.random.uniform(jax.random.fold_in(jax.random.fold_in(own_key, 6), dim), (blocks,), jnp.float32, least / len(shards), high / len(shards))
        factor_of = factor_of * jnp.repeat(jnp.exp(draws), dims[dim] // blocks).reshape((-1,) + (1,) * (len(dims) - 1 - dim))
    return factor_of


def routed_block(own_key, own, number, rows, amount, top, most, slope):
    order = jax.random.permutation(own_key, amount)
    packed, ordinary = load_shares(amount, rows * top, most, slope, True), load_shares(amount, rows * top, most, slope, False)
    places = jnp.arange(amount)

    def named(sizes, rotation):
        used = int((sizes > 0).sum())
        fixed = max(1, used // 4)
        moved = fixed + (places - fixed + rotation * (used - fixed)) % max(1, amount - fixed)
        return jnp.zeros((amount,), jnp.int32).at[order[jnp.where(places < fixed, places, moved)]].set(jnp.asarray(sizes, jnp.int32))

    sizes = jnp.where(number % 4 == 0, named(packed, number // 4), named(ordinary, number - number // 4 - 1))
    mixed = jax.random.permutation(jax.random.fold_in(own, 3), amount)
    donor, sink = mixed[0:amount // 2 * 2:2], mixed[1:amount // 2 * 2:2]
    margin = jnp.minimum(sizes[donor] - 1, most - sizes[sink]) // 2
    margin = jnp.where((donor == order[0]) | (sink == order[0]) | (sizes[sink] == 0), 0, jnp.maximum(margin, 0))
    moved = jax.random.randint(jax.random.fold_in(own, 4), (amount // 2,), 0, 1 << 20) % (margin + 1)
    sizes = sizes.at[donor].add(-moved).at[sink].add(moved)
    members = jnp.searchsorted(jnp.cumsum(sizes), jnp.arange(rows * top), side="right").astype(jnp.int32)
    listing = members.reshape(top, rows).T
    listing = listing[jax.random.permutation(jax.random.fold_in(own, 1), rows)]
    rotation = jax.random.randint(jax.random.fold_in(own, 2), (rows, 1), 0, top)
    return jnp.take_along_axis(listing, (jnp.arange(top)[None, :] + rotation) % top, axis=1)


def load_shares(amount, total, most, skew, full):
    weights = [(1 << 20) // math.isqrt(standing ** skew) + 1 for standing in range(1, amount + 1)]
    largest = most if full else min(most, max(-(-total // amount), total * weights[0] // sum(weights)))
    least = 1 if total - largest >= amount - 1 else 0
    given, surplus = [largest] + [least] * (amount - 1), total - largest - least * (amount - 1)
    while surplus > 0:
        movable = [i for i in range(1, amount) if given[i] < largest] or [i for i in range(1, amount) if given[i] < most]
        whole, left = sum([weights[i] for i in movable]), surplus
        for i in movable:
            addition = min(most - given[i], max(1, left * weights[i] // whole), surplus)
            given[i] = given[i] + addition
            surplus = surplus - addition
    return np.array(given)


def scatter_about(rng, shape, scale, bound, pieces=(), held_as=jnp.bfloat16):
    entries = scale * jax.random.normal(rng, shape, jnp.float32)
    if pieces:
        entries = entries * levels(rng, shape, pieces, -0.22, 0.18)
    return jnp.clip(entries, -bound, bound).astype(held_as)


def setup_inputs(seed: int = 0) -> dict:
    splits = jax.random.split(jax.random.key(seed), 15)
    mix_input = scatter_about(splits[0], (TOKENS_A, D), 1.0, 6.0, ((0, 256),))
    mix_gain = jnp.clip(1.0 + 0.18 * jax.random.normal(splits[1], (D,), jnp.float32), 0.1, 1.9)
    pool_weight = scatter_about(splits[2], (4, GROUP, GROUP), GROUP ** -0.5, 0.25)
    pool_scale = jnp.clip(1.0 + 0.18 * jax.random.normal(splits[3], (D,), jnp.float32), 0.1, 1.9)
    moe_input = scatter_about(splits[4], (TOKENS_B, D), 1.0, 6.0, ((0, 256),))
    moe_gain = jnp.clip(1.0 + 0.18 * jax.random.normal(splits[5], (D,), jnp.float32), 0.1, 1.9)
    expert_ids_keys = jax.random.split(jax.random.fold_in(splits[6], 1), TOKENS_B // TOK_B)
    expert_ids_turns = jax.random.permutation(jax.random.fold_in(splits[6], 3), TOKENS_B // TOK_B)
    expert_ids = jax.vmap(lambda own, number: routed_block(jax.random.fold_in(splits[6], 2), own, number, TOK_B, EXPERTS, TOPK, CAP, 1))(expert_ids_keys, expert_ids_turns).reshape((TOKENS_B, TOPK))
    route_score = jnp.clip(jnp.exp(math.log(1.0) - 2.9957323 * jax.random.uniform(splits[7], (TOKENS_B, TOPK), jnp.float32) ** levels(splits[7], (TOKENS_B, TOPK), ((0, 256),), -0.2, 0.2)), 0.05, 1.0)
    expert_gate = scatter_about(splits[8], (EXPERTS, D, FF), D ** -0.5, 0.125, ((0, 64), (2, 4)))
    expert_up = scatter_about(splits[9], (EXPERTS, D, FF), D ** -0.5, 0.125, ((0, 64), (2, 4)))
    expert_down = scatter_about(splits[10], (EXPERTS, FF, D), FF ** -0.5, 0.1875, ((0, 64), (1, 4)))
    shared_gate = scatter_about(splits[11], (D, SH), D ** -0.5, 0.125, ((1, 4),))
    shared_up = scatter_about(splits[12], (D, SH), D ** -0.5, 0.125, ((1, 4),))
    shared_down = scatter_about(splits[13], (SH, D), SH ** -0.5, 0.25, ((0, 4),))
    return dict(mix_input=mix_input, mix_gain=mix_gain, pool_weight=pool_weight, pool_scale=pool_scale, moe_input=moe_input, moe_gain=moe_gain, expert_ids=expert_ids, route_score=route_score, expert_gate=expert_gate, expert_up=expert_up, expert_down=expert_down, shared_gate=shared_gate, shared_up=shared_up, shared_down=shared_down)


WINDOWS = (2, 4, 8, 16)
RMS_EPS = 1e-06
ROUTED_SCALE = 2.5

def rms_norm(values, gain_row):
    upcast = values.astype(jnp.float32)
    scaled = upcast * lax.rsqrt(lax.optimization_barrier(jnp.mean(upcast * upcast, axis=-1, keepdims=True)) + RMS_EPS)
    return (scaled * gain_row).astype(jnp.bfloat16)

def rounded(values):
    return lax.optimization_barrier(values.astype(jnp.bfloat16)).astype(jnp.float32)

def window_means(normed, before, offset):
    row_count = normed.shape[0]
    lead_rows = before.shape[0]
    group_size = normed.shape[1] // len(WINDOWS)
    joined = jnp.concatenate([before, normed], axis=0).astype(jnp.float32)
    positions = offset + jnp.arange(row_count, dtype=jnp.int32)
    window_avg = []
    for group_idx, span in enumerate(WINDOWS):
        channels = joined[:, group_idx * group_size:(group_idx + 1) * group_size]
        first_row = lead_rows - span + 1
        running = channels[first_row:first_row + row_count]
        for shift_idx in range(1, span):
            running = running + channels[first_row + shift_idx:first_row + shift_idx + row_count]
        counts = jnp.minimum(positions + 1, span).astype(jnp.float32)
        window_avg.append(running / counts[:, None])
    return jnp.stack(window_avg, axis=1)

def width_sum(hidden, down_rows, block_width):
    summed = jnp.zeros((hidden.shape[0], down_rows.shape[1]), jnp.float32)
    for part_idx in range(N_TP):
        piece_out = jnp.dot(hidden[:, part_idx * block_width:(part_idx + 1) * block_width], down_rows[part_idx * block_width:(part_idx + 1) * block_width], preferred_element_type=jnp.float32)
        summed = summed + rounded(piece_out)
    return summed.astype(jnp.bfloat16)

def reference(mix_input, mix_gain, pool_weight, pool_scale, moe_input, moe_gain, expert_ids, route_score, expert_gate, expert_up, expert_down, shared_gate, shared_up, shared_down):
    normed = rms_norm(mix_input, mix_gain)
    row_count, width_all = normed.shape
    reach_rows = max(WINDOWS) - 1
    before = jnp.zeros((reach_rows, width_all), jnp.bfloat16)
    pooled = window_means(normed, before, 0)
    difference = (pooled - normed.astype(jnp.float32).reshape(row_count, len(WINDOWS), -1)).astype(jnp.bfloat16)
    mixed_out = jnp.einsum('sgc,gcd->sgd', difference.astype(jnp.float32), pool_weight.astype(jnp.float32))
    mix_output = (mixed_out.reshape(row_count, width_all) * pool_scale).astype(jnp.bfloat16)
    tok_count = moe_input.shape[0]
    h_moe = rms_norm(moe_input, moe_gain)
    block_count = tok_count // TOK_B
    pair_ids = expert_ids.reshape(block_count, TOK_B * TOPK)
    onehot = (pair_ids[:, :, None] == jnp.arange(EXPERTS, dtype=jnp.int32)[None, None, :]).astype(jnp.int32)
    rank = lax.optimization_barrier(jnp.sum((jnp.cumsum(onehot, axis=1) - onehot) * onehot, axis=2))
    block_idx = jnp.arange(block_count, dtype=jnp.int32)[:, None]
    slot_col = block_idx * CAP + rank
    owner = block_idx * TOK_B + jnp.arange(TOK_B * TOPK, dtype=jnp.int32)[None, :] // TOPK
    table = jnp.full((EXPERTS, block_count * CAP), tok_count, jnp.int32).at[pair_ids, slot_col].set(owner)
    padded = jnp.concatenate([h_moe, jnp.zeros((1, D), jnp.bfloat16)], axis=0)

    def run_expert(index):
        picked = padded[table[index]]
        gate_val = jnp.dot(picked, expert_gate[index], preferred_element_type=jnp.float32)
        up_val = jnp.dot(picked, expert_up[index], preferred_element_type=jnp.float32)
        hidden = (jax.nn.silu(gate_val) * up_val).astype(jnp.bfloat16)
        return width_sum(hidden, expert_down[index], FF // N_TP)
    results = lax.map(run_expert, jnp.arange(EXPERTS, dtype=jnp.int32))
    flat_res = results.reshape(EXPERTS * block_count * CAP, D)
    flat_idx = (pair_ids * (block_count * CAP) + slot_col).reshape(tok_count, TOPK)
    shared_gate_val = jnp.dot(h_moe, shared_gate, preferred_element_type=jnp.float32)
    shared_up_val = jnp.dot(h_moe, shared_up, preferred_element_type=jnp.float32)
    shared_hidden = (jax.nn.silu(shared_gate_val) * shared_up_val).astype(jnp.bfloat16)
    shared_out = width_sum(shared_hidden, shared_down, SH // N_TP)
    route_w = route_score / lax.optimization_barrier(jnp.sum(route_score, axis=1, keepdims=True)) * ROUTED_SCALE
    combined = shared_out.astype(jnp.float32)
    for pick_idx in range(TOPK):
        combined = combined + route_w[:, pick_idx:pick_idx + 1] * flat_res[flat_idx[:, pick_idx]].astype(jnp.float32)
    return (mix_output, combined.astype(jnp.bfloat16))
```

```python
import jax
import jax.numpy as jnp
import numpy as np
from jax import lax
from jax.experimental import pallas as pl
from jax.experimental.pallas import tpu as pltpu
from jax.sharding import PartitionSpec as P


WINDOWS = (2, 4, 8, 16)
RMS_EPS = 1e-06
ROUTED_SCALE = 2.5
CAP = 6
COLS = 4
PACK = CAP * COLS
BLOCK = 8
PAIR_A = ((0, 1), (1, 0), (2, 3), (3, 2))
PAIR_B = ((1, 2), (2, 1), (3, 0), (0, 3))


f32 = jnp.float32
bf16 = jnp.bfloat16


def dot32(a, b):
    return jnp.dot(a, b, preferred_element_type=f32)


def call(body, out, scratch=(), smem=(), count=0, plane=None):
    def spec(i):
        if plane and i in plane:
            at, shape = plane[i]
            return pl.BlockSpec((None, *shape), lambda _: (at, 0, 0))
        return pl.BlockSpec(memory_space=pltpu.SMEM if i in smem else pltpu.VMEM)

    return pl.pallas_call(
        body,
        out_shape=out,
        grid=(1,) if plane else (),
        in_specs=[spec(i) for i in range(count)],
        scratch_shapes=list(scratch),
    )


def unpack_matrix():
    rows = BLOCK * PACK
    per = BLOCK * CAP
    place = np.zeros((rows, rows), np.float32)
    for i in range(rows):
        q, rest = divmod(i, per)
        j, s = divmod(rest, CAP)
        place[i, j * PACK + q * CAP + s] = 1.0
    return place


def dispatch_body(x_ref, gain_ref, ids_ref, h_ref, m0_ref, m1_ref, rank_ref, hcat_ref):
    x = x_ref[...].astype(f32)
    mean = jnp.mean(x * x, axis=-1, keepdims=True)
    h = (x * lax.rsqrt(mean + RMS_EPS) * gain_ref[...]).astype(bf16)
    h_ref[...] = h
    toks, width = h.shape
    part = width // COLS
    for q in range(COLS):
        hcat_ref[q * toks : (q + 1) * toks, :] = h[:, q * part : (q + 1) * part]
    peers = rank_ref.shape[0]
    before = (
        lax.broadcasted_iota(jnp.int32, (toks, toks), 0)
        < lax.broadcasted_iota(jnp.int32, (toks, toks), 1)
    ).astype(f32).astype(bf16)
    for e, m_ref in enumerate((m0_ref, m1_ref)):
        expert = 2 * lax.broadcasted_iota(jnp.int32, (peers, toks), 0) + e
        named = jnp.zeros((peers, toks), f32)
        for k in range(ids_ref.shape[0]):
            named = named + (ids_ref[k : k + 1, :] == expert).astype(f32)
        rank = dot32(named.astype(bf16), before)
        rank = jnp.where(named > 0, rank, -1.0)
        for q in range(COLS):
            rank_ref[:, q * toks : (q + 1) * toks] = rank

        def block(b, _):
            ranks = rank_ref[pl.ds(pl.multiple_of(b * BLOCK, BLOCK), BLOCK), :]
            shape = (BLOCK, PACK, COLS * toks)
            r = lax.broadcasted_iota(jnp.int32, shape, 1)
            col = lax.broadcasted_iota(jnp.int32, shape, 2)
            q = sum((r >= CAP * i).astype(jnp.int32) for i in range(1, COLS))
            want = jnp.where(
                (col >= q * toks) & (col < (q + 1) * toks), (r - CAP * q).astype(f32), -2.0
            )
            pick = (jnp.broadcast_to(ranks[:, None, :], shape) == want).astype(f32)
            pick = pick.reshape(BLOCK * PACK, COLS * toks).astype(bf16)
            rows = BLOCK * PACK
            m_ref[pl.ds(pl.multiple_of(b * rows, rows), rows), :] = dot32(
                pick, hcat_ref[...]
            ).astype(bf16)
            return 0

        lax.fori_loop(0, peers // BLOCK, block, 0)


def unpack_into(x_ref, place_ref, rows_ref):
    rows = BLOCK * PACK
    per = BLOCK * CAP
    part = x_ref.shape[1]

    def block(b, _):
        got = dot32(
            place_ref[...], x_ref[pl.ds(pl.multiple_of(b * rows, rows), rows), :]
        ).astype(bf16)
        for q in range(COLS):
            rows_ref[
                pl.ds(pl.multiple_of(b * per, per), per), q * part : (q + 1) * part
            ] = got[q * per : (q + 1) * per, :]
        return 0

    lax.fori_loop(0, x_ref.shape[0] // rows, block, 0)


def hidden_body(x_ref, place_ref, ga_ref, ua_ref, gb_ref, ub_ref, hid_ref, rows_ref):
    unpack_into(x_ref, place_ref, rows_ref)
    x = rows_ref[...]
    w = ga_ref.shape[-1]
    for i, (g_ref, u_ref) in enumerate(((ga_ref, ua_ref), (gb_ref, ub_ref))):
        gate = dot32(x, g_ref[...])
        up = dot32(x, u_ref[...])
        hid_ref[:, i * w : (i + 1) * w] = (gate / (1.0 + jnp.exp(-gate)) * up).astype(bf16)


def down_body(mine_ref, theirs_ref, d0_ref, d1_ref, d2_ref, d3_ref, place_ref, out_ref, y_ref):
    w = mine_ref.shape[1] // 2
    total = dot32(mine_ref[:, :w], d0_ref[...]) + dot32(mine_ref[:, w:], d1_ref[...])
    total = total + dot32(theirs_ref[:, :w], d2_ref[...]) + dot32(theirs_ref[:, w:], d3_ref[...])
    y_ref[...] = total.astype(bf16)
    rows = BLOCK * PACK
    per = BLOCK * CAP
    part = out_ref.shape[1]

    def block(b, _):
        at = pl.ds(pl.multiple_of(b * per, per), per)
        stack = jnp.concatenate(
            [y_ref[at, q * part : (q + 1) * part] for q in range(COLS)], axis=0
        )
        out_ref[pl.ds(pl.multiple_of(b * rows, rows), rows), :] = dot32(
            place_ref[...], stack
        ).astype(bf16)
        return 0

    lax.fori_loop(0, y_ref.shape[0] // per, block, 0)


def combine_body(e, ids_ref, score_ref, base_ref, r_ref, place_ref, out_ref, rows_ref):
    unpack_into(r_ref, place_ref, rows_ref)
    toks = ids_ref.shape[0]
    total = rows_ref.shape[0]
    peers = total // CAP
    score = score_ref[...]
    weight = score / jnp.sum(score, axis=1, keepdims=True) * ROUTED_SCALE
    expert = 2 * lax.broadcasted_iota(jnp.int32, (toks, peers), 1) + e
    named = jnp.zeros((toks, peers), f32)
    scaled = jnp.zeros((toks, peers), f32)
    for k in range(ids_ref.shape[1]):
        hit = ids_ref[:, k : k + 1] == expert
        named = named + hit.astype(f32)
        scaled = scaled + jnp.where(hit, weight[:, k : k + 1], 0.0)
    before = (
        lax.broadcasted_iota(jnp.int32, (toks, toks), 1)
        < lax.broadcasted_iota(jnp.int32, (toks, toks), 0)
    ).astype(f32).astype(bf16)
    rank = jnp.where(named > 0, dot32(before, named.astype(bf16)), -1.0).astype(bf16)
    at = lax.broadcasted_iota(jnp.int32, (peers, total), 1) - CAP * lax.broadcasted_iota(
        jnp.int32, (peers, total), 0
    )
    mine = (at >= 0) & (at < CAP)
    spread = mine.astype(f32).astype(bf16)
    slot = jnp.sum(jnp.where(mine, at, 0).astype(f32), axis=0, keepdims=True)
    here = dot32(rank, spread) == slot
    high = scaled.astype(bf16)
    low = (scaled - high.astype(f32)).astype(bf16)
    acc = base_ref[...].astype(f32)
    for piece in (high, low):
        lhs = jnp.where(here, dot32(piece, spread), 0.0).astype(bf16)
        acc = acc + dot32(lhs, rows_ref[...])
    out_ref[...] = acc.astype(out_ref.dtype)


def rms_norm(values, gain_row):
    upcast = values.astype(f32)
    scaled = upcast * lax.rsqrt(jnp.mean(upcast * upcast, axis=-1, keepdims=True) + RMS_EPS)
    return (scaled * gain_row).astype(bf16)


def mixer_body(at_ref, x_ref, gain_ref, halo_ref, pool_ref, scale_ref, out_ref, rows_ref):
    lead = halo_ref.shape[0]
    rows, width = x_ref.shape
    group = width // len(WINDOWS)
    rows_ref[:lead, :] = halo_ref[...]
    rows_ref[lead:, :] = rms_norm(x_ref[...], gain_ref[...])
    ahead = lax.broadcasted_iota(jnp.int32, (rows, lead + rows), 0) + lead
    back = ahead - lax.broadcasted_iota(jnp.int32, (rows, lead + rows), 1)
    taken = at_ref[0] + 1 + lax.broadcasted_iota(jnp.int32, (rows, 1), 0)
    for g, span in enumerate(WINDOWS):
        cols = slice(g * group, (g + 1) * group)
        band = ((back >= 0) & (back < span)).astype(f32).astype(bf16)
        pooled = dot32(band, rows_ref[:, cols]) / jnp.minimum(taken, span).astype(f32)
        difference = (pooled - rows_ref[lead:, cols].astype(f32)).astype(bf16)
        out_ref[:, cols] = (dot32(difference, pool_ref[g]) * scale_ref[:, cols]).astype(bf16)


def tail_before(mix_input, mix_gain):
    lead = max(WINDOWS)
    length = lax.axis_size(("ep", "tp"))
    return lax.ppermute(
        rms_norm(mix_input[mix_input.shape[0] - lead :], mix_gain),
        ("ep", "tp"),
        [(i, i + 1) for i in range(length - 1)],
    )


def mixer(mix_input, mix_gain, before, pool_weight, pool_scale):
    rows, width = mix_input.shape
    lead = before.shape[0]
    offset = (lax.axis_index(("ep", "tp")) * rows).astype(jnp.int32)
    return call(
        mixer_body,
        jax.ShapeDtypeStruct((rows, width), bf16),
        (pltpu.VMEM((lead + rows, width), bf16),),
        smem=(0,),
        count=6,
    )(offset[None], mix_input, mix_gain[None, :], before, pool_weight, pool_scale[None, :])


def layer(
    mix_input,
    mix_gain,
    pool_weight,
    pool_scale,
    moe_input,
    moe_gain,
    expert_ids,
    route_score,
    expert_gate,
    expert_up,
    expert_down,
    shared_gate,
    shared_up,
    shared_down,
):
    toks, width = moe_input.shape
    peers = lax.axis_size("ep")
    quarter = lax.axis_index("tp")
    part = width // COLS
    packed = peers * PACK
    slots = peers * CAP
    place = jnp.asarray(unpack_matrix(), bf16)
    place_back = jnp.asarray(unpack_matrix().T, bf16)
    my_ids = lax.dynamic_slice_in_dim(expert_ids, quarter * toks, toks, 0)

    pairs = (PAIR_A, PAIR_B)

    def swap(value, pairs):
        return lax.ppermute(value, "tp", pairs)

    pairs = (PAIR_A, PAIR_B)
    gates = [swap(expert_gate[e], pairs[e]) for e in range(2)]
    ups = [swap(expert_up[e], pairs[e]) for e in range(2)]
    down_a = swap(expert_down, PAIR_A)
    down_b = [swap(expert_down[e], PAIR_B) for e in range(2)]
    across = [swap(down_b[0], PAIR_A), swap(down_a[1], PAIR_B)]

    h, *sends = call(
        dispatch_body,
        (
            jax.ShapeDtypeStruct((toks, width), bf16),
            jax.ShapeDtypeStruct((packed, part), bf16),
            jax.ShapeDtypeStruct((packed, part), bf16),
        ),
        (pltpu.VMEM((peers, COLS * toks), f32), pltpu.VMEM((COLS * toks, part), bf16)),
        count=3,
    )(moe_input, moe_gain[None, :], my_ids.T)

    def over_ep(value):
        value = value.reshape(peers, PACK, part)
        return lax.all_to_all(value, "ep", 0, 0, tiled=True).reshape(packed, part)

    def hidden_half(rows, e):
        return call(
            hidden_body,
            jax.ShapeDtypeStruct((slots, 2 * expert_gate.shape[2]), bf16),
            (pltpu.VMEM((slots, width), bf16),),
            count=6,
            plane={i: (e, expert_gate.shape[1:]) for i in (2, 3)},
        )(rows, place, expert_gate, expert_up, gates[e], ups[e])

    back = []
    for e in range(2):
        own = over_ep(sends[e])
        other = swap(own, pairs[1 - e])
        mine = hidden_half(own, e)
        theirs = hidden_half(other, e)
        theirs = swap(theirs, pairs[1 - e])
        whole = (e, expert_down.shape[1:])
        weights = (expert_down, down_a, down_b[0], across[0])
        planes = {2: whole, 3: whole}
        if e == 1:
            weights = (expert_down, down_b[1], down_a, across[1])
            planes = {2: whole, 4: whole}
        back.append(
            call(
                down_body,
                jax.ShapeDtypeStruct((packed, part), bf16),
                (pltpu.VMEM((slots, width), bf16),),
                count=7,
                plane=planes,
            )(mine, theirs, *weights, place_back)
        )

    everyone = lax.all_gather(h, "tp", axis=0, tiled=True)
    shared_hidden = (
        jax.nn.silu(dot32(everyone, shared_gate)) * dot32(everyone, shared_up)
    ).astype(bf16)
    shared_part = dot32(shared_hidden, shared_down).astype(bf16)
    acc = lax.psum_scatter(shared_part, "tp", scatter_dimension=0, tiled=True)

    halo = tail_before(mix_input, mix_gain)
    mix_output = mixer(mix_input, mix_gain, halo, pool_weight, pool_scale)

    for e in range(2):
        returned = over_ep(back[e])
        acc = call(
            lambda *refs, e=e: combine_body(e, *refs),
            jax.ShapeDtypeStruct((toks, width), bf16 if e == 1 else f32),
            (pltpu.VMEM((slots, width), bf16),),
            count=5,
        )(my_ids, route_score, acc, returned, place)
    return (mix_output, acc)


def solution(mesh):
    return jax.shard_map(
        layer,
        mesh=mesh,
        in_specs=(
            P(("ep", "tp"), None),
            P(),
            P(),
            P(),
            P(("ep", "tp"), None),
            P(),
            P("ep", None),
            P(("ep", "tp"), None),
            P("ep", None, "tp"),
            P("ep", None, "tp"),
            P("ep", "tp", None),
            P(None, "tp"),
            P(None, "tp"),
            P("tp", None),
        ),
        out_specs=(P(("ep", "tp"), None), P(("ep", "tp"), None)),
        check_vma=False,
    )
```

```python
import functools

import jax
import jax.numpy as jnp
import numpy as np
from jax import lax
from jax.experimental import pallas as pl
from jax.experimental.pallas import tpu as pltpu
from jax.sharding import PartitionSpec as P


WINDOWS = (2, 4, 8, 16)
RMS_EPS = 1e-06
ROUTED_SCALE = 2.5
CAP = 6
COLS = 4
PACK = CAP * COLS
BLOCK = 8
SEND_BLOCK = 16
PAIR_A = ((0, 1), (1, 0), (2, 3), (3, 2))
PAIR_B = ((1, 2), (2, 1), (3, 0), (0, 3))


f32 = jnp.float32
bf16 = jnp.bfloat16


def dot32(a, b):
    return jnp.dot(a, b, preferred_element_type=f32)


def call(body, out, scratch=(), count=0, smem=(), hbm=()):
    def spec(i):
        if i in hbm:
            return pl.BlockSpec(memory_space=pltpu.HBM)
        return pl.BlockSpec(memory_space=pltpu.SMEM if i in smem else pltpu.VMEM)

    return pl.pallas_call(
        body, out_shape=out, in_specs=[spec(i) for i in range(count)], scratch_shapes=list(scratch)
    )


def unpack_matrix():
    rows = BLOCK * PACK
    per = BLOCK * CAP
    place = np.zeros((rows, rows), np.float32)
    for i in range(rows):
        q, rest = divmod(i, per)
        j, s = divmod(rest, CAP)
        place[i, j * PACK + q * CAP + s] = 1.0
    return place


def norm_send_body(at_ref, x_ref, gain_ref, ids_ref, h_ref, m_ref, rank_ref, hcat_ref):
    h_ref[...] = rms_norm(x_ref[...], gain_ref[...])
    send_rows(0, at_ref, h_ref, ids_ref, m_ref, rank_ref, hcat_ref)


def send_body(at_ref, h_ref, ids_ref, m_ref, rank_ref, hcat_ref):
    send_rows(1, at_ref, h_ref, ids_ref, m_ref, rank_ref, hcat_ref)


def send_rows(e, at_ref, h_ref, ids_ref, m_ref, rank_ref, hcat_ref):
    toks, width = h_ref.shape
    part = width // COLS
    for q in range(COLS):
        hcat_ref[q * toks : (q + 1) * toks, :] = h_ref[:, q * part : (q + 1) * part]
    peers = rank_ref.shape[0]
    ids = ids_ref[:, pl.ds(pl.multiple_of(at_ref[0] * toks, toks), toks)]
    expert = 2 * lax.broadcasted_iota(jnp.int32, (peers, toks), 0) + e
    named = jnp.zeros((peers, toks), f32)
    for k in range(ids.shape[0]):
        named = named + (ids[k : k + 1, :] == expert).astype(f32)
    before = (
        lax.broadcasted_iota(jnp.int32, (toks, toks), 0)
        < lax.broadcasted_iota(jnp.int32, (toks, toks), 1)
    ).astype(f32).astype(bf16)
    rank = jnp.where(named > 0, dot32(named.astype(bf16), before), -1.0)
    for q in range(COLS):
        rank_ref[:, q * toks : (q + 1) * toks] = rank

    def block(b, _):
        ranks = rank_ref[pl.ds(pl.multiple_of(b * SEND_BLOCK, SEND_BLOCK), SEND_BLOCK), :]
        shape = (SEND_BLOCK, PACK, COLS * toks)
        r = lax.broadcasted_iota(jnp.int32, shape, 1)
        col = lax.broadcasted_iota(jnp.int32, shape, 2)
        q = sum((r >= CAP * i).astype(jnp.int32) for i in range(1, COLS))
        want = jnp.where(
            (col >= q * toks) & (col < (q + 1) * toks), (r - CAP * q).astype(f32), -2.0
        )
        pick = (jnp.broadcast_to(ranks[:, None, :], shape) == want).astype(f32)
        pick = pick.reshape(SEND_BLOCK * PACK, COLS * toks).astype(bf16)
        rows = SEND_BLOCK * PACK
        m_ref[pl.ds(pl.multiple_of(b * rows, rows), rows), :] = dot32(
            pick, hcat_ref[...]
        ).astype(bf16)
        return 0

    lax.fori_loop(0, peers // SEND_BLOCK, block, 0)


def fetch(sources, targets, sems):
    copies = [
        pltpu.make_async_copy(src, dst, sems.at[i])
        for i, (src, dst) in enumerate(zip(sources, targets))
    ]
    for copy in copies:
        copy.start()
    return copies


def plane(ref, e):
    return ref.at[e] if len(ref.shape) == 3 else ref


def unpack_into(x_ref, place_ref, rows_ref):
    rows = BLOCK * PACK
    per = BLOCK * CAP
    part = x_ref.shape[1]

    def block(b, _):
        got = dot32(
            place_ref[...], x_ref[pl.ds(pl.multiple_of(b * rows, rows), rows), :]
        ).astype(bf16)
        for q in range(COLS):
            rows_ref[
                pl.ds(pl.multiple_of(b * per, per), per), q * part : (q + 1) * part
            ] = got[q * per : (q + 1) * per, :]
        return 0

    lax.fori_loop(0, x_ref.shape[0] // rows, block, 0, unroll=4)


def hidden_body(e, x_ref, place_ref, ga, ua, ub, *refs):
    *gb, hid_ref, rows_ref, held_ref, sems = refs
    w = held_ref.shape[1] // 4
    tall = held_ref.shape[0] // len(gb)
    targets = [held_ref.at[:, i * w : (i + 1) * w] for i in (0, 2, 3)]
    targets += [held_ref.at[i * tall : (i + 1) * tall, w : 2 * w] for i in range(len(gb))]
    copies = fetch([plane(ref, e) for ref in (ga, ua, ub, *gb)], targets, sems)
    unpack_into(x_ref, place_ref, rows_ref)
    for copy in copies:
        copy.wait()
    both = dot32(rows_ref[...], held_ref[...])
    gate = both[:, : 2 * w]
    hid_ref[...] = (gate / (1.0 + jnp.exp(-gate)) * both[:, 2 * w :]).astype(bf16)


def down_body(
    e, mine_ref, theirs_ref, d0, d1, d2, d3, place_ref, out_ref, y_ref, held_ref, hid_ref, sems
):
    w = mine_ref.shape[1] // 2
    cols = held_ref.shape[1] // 2
    sides = [slice(c * cols, (c + 1) * cols) for c in range(2)]
    copies = [
        fetch(
            [plane(ref, e).at[:, side] for ref in (d0, d1, d2, d3)],
            [held_ref.at[i * w : (i + 1) * w, side] for i in range(4)],
            sems.at[pl.ds(4 * c, 4)],
        )
        for c, side in enumerate(sides)
    ]
    hid_ref[:, : 2 * w] = mine_ref[...]
    hid_ref[:, 2 * w :] = theirs_ref[...]
    for side, group in zip(sides, copies):
        for copy in group:
            copy.wait()
        y_ref[:, side] = dot32(hid_ref[...], held_ref[:, side]).astype(bf16)
    rows = BLOCK * PACK
    per = BLOCK * CAP
    part = out_ref.shape[1]

    def block(b, _):
        at = pl.ds(pl.multiple_of(b * per, per), per)
        stack = jnp.concatenate(
            [y_ref[at, q * part : (q + 1) * part] for q in range(COLS)], axis=0
        )
        out_ref[pl.ds(pl.multiple_of(b * rows, rows), rows), :] = dot32(
            place_ref[...], stack
        ).astype(bf16)
        return 0

    lax.fori_loop(0, y_ref.shape[0] // per, block, 0, unroll=4)


def route_matrix(e, ids, score, peers):
    toks = ids.shape[0]
    total = peers * CAP
    weight = score / jnp.sum(score, axis=1, keepdims=True) * ROUTED_SCALE
    expert = 2 * lax.broadcasted_iota(jnp.int32, (toks, peers), 1) + e
    named = jnp.zeros((toks, peers), f32)
    scaled = jnp.zeros((toks, peers), f32)
    for k in range(ids.shape[1]):
        hit = ids[:, k : k + 1] == expert
        named = named + hit.astype(f32)
        scaled = scaled + jnp.where(hit, weight[:, k : k + 1], 0.0)
    before = (
        lax.broadcasted_iota(jnp.int32, (toks, toks), 1)
        < lax.broadcasted_iota(jnp.int32, (toks, toks), 0)
    ).astype(f32).astype(bf16)
    rank = jnp.where(named > 0, dot32(before, named.astype(bf16)), -1.0).astype(bf16)
    at = lax.broadcasted_iota(jnp.int32, (peers, total), 1) - CAP * lax.broadcasted_iota(
        jnp.int32, (peers, total), 0
    )
    mine = (at >= 0) & (at < CAP)
    spread = mine.astype(f32).astype(bf16)
    slot = jnp.sum(jnp.where(mine, at, 0).astype(f32), axis=0, keepdims=True)
    here = dot32(rank, spread) == slot
    high = scaled.astype(bf16)
    low = (scaled - high.astype(f32)).astype(bf16)
    return [jnp.where(here, dot32(piece, spread), 0.0).astype(bf16) for piece in (high, low)]


def first_body(
    at_ref, ids_ref, score_ref, base_ref, r_ref, place_ref, acc_ref, route_ref, rows_ref
):
    unpack_into(r_ref, place_ref, rows_ref)
    score = score_ref[...]
    toks = score.shape[0]
    ids = ids_ref[pl.ds(pl.multiple_of(at_ref[0] * toks, toks), toks), :]
    peers = rows_ref.shape[0] // CAP
    acc = base_ref[...]
    for piece in route_matrix(0, ids, score, peers):
        acc = acc + dot32(piece, rows_ref[...])
    acc_ref[...] = acc
    route_ref[:toks, :], route_ref[toks:, :] = route_matrix(1, ids, score, peers)


def last_body(acc_ref, more_ref, route_ref, r_ref, place_ref, out_ref, rows_ref):
    unpack_into(r_ref, place_ref, rows_ref)
    toks = acc_ref.shape[0]
    both = dot32(route_ref[...], rows_ref[...])
    acc = acc_ref[...] + more_ref[...].astype(f32) + both[:toks] + both[toks:]
    out_ref[...] = acc.astype(bf16)


def shared_body(own_ref, other_ref, ga, ua, da, gb, ub, db, own_out_ref, other_out_ref):
    for h_ref, out_ref in ((other_ref, other_out_ref), (own_ref, own_out_ref)):
        h = h_ref[...]
        total = None
        for g_ref, u_ref, d_ref in ((ga, ua, da), (gb, ub, db)):
            gate = dot32(h, g_ref[...])
            up = dot32(h, u_ref[...])
            hidden = (gate / (1.0 + jnp.exp(-gate)) * up).astype(bf16)
            piece = dot32(hidden, d_ref[...])
            total = piece if total is None else total + piece
        out_ref[...] = total.astype(out_ref.dtype)


def rms_norm(values, gain_row):
    upcast = values.astype(f32)
    scaled = upcast * lax.rsqrt(jnp.mean(upcast * upcast, axis=-1, keepdims=True) + RMS_EPS)
    return (scaled * gain_row).astype(bf16)


def mixer_body(at_ref, x_ref, gain_ref, halo_ref, pool_ref, scale_ref, out_ref, rows_ref):
    lead = halo_ref.shape[0]
    rows, width = x_ref.shape
    group = width // len(WINDOWS)
    rows_ref[:lead, :] = halo_ref[...]
    rows_ref[lead:, :] = rms_norm(x_ref[...], gain_ref[...])
    ahead = lax.broadcasted_iota(jnp.int32, (rows, lead + rows), 0) + lead
    back = ahead - lax.broadcasted_iota(jnp.int32, (rows, lead + rows), 1)
    taken = at_ref[0] + 1 + lax.broadcasted_iota(jnp.int32, (rows, 1), 0)
    for g, span in enumerate(WINDOWS):
        cols = slice(g * group, (g + 1) * group)
        band = ((back >= 0) & (back < span)).astype(f32).astype(bf16)
        pooled = dot32(band, rows_ref[:, cols]) / jnp.minimum(taken, span).astype(f32)
        difference = (pooled - rows_ref[lead:, cols].astype(f32)).astype(bf16)
        out_ref[:, cols] = (dot32(difference, pool_ref[g]) * scale_ref[:, cols]).astype(bf16)


def tail_before(mix_input, mix_gain):
    lead = max(WINDOWS)
    length = lax.axis_size(("ep", "tp"))
    return lax.ppermute(
        rms_norm(mix_input[mix_input.shape[0] - lead :], mix_gain),
        ("ep", "tp"),
        [(i, i + 1) for i in range(length - 1)],
    )


def mixer(mix_input, mix_gain, before, pool_weight, pool_scale):
    rows, width = mix_input.shape
    lead = before.shape[0]
    offset = (lax.axis_index(("ep", "tp")) * rows).astype(jnp.int32)
    return call(
        mixer_body,
        jax.ShapeDtypeStruct((rows, width), bf16),
        (pltpu.VMEM((lead + rows, width), bf16),),
        smem=(0,),
        count=6,
    )(offset[None], mix_input, mix_gain[None, :], before, pool_weight, pool_scale[None, :])


def layer(
    mix_input,
    mix_gain,
    pool_weight,
    pool_scale,
    moe_input,
    moe_gain,
    expert_ids,
    route_score,
    expert_gate,
    expert_up,
    expert_down,
    shared_gate,
    shared_up,
    shared_down,
):
    toks, width = moe_input.shape
    peers = lax.axis_size("ep")
    quarter = lax.axis_index("tp")
    part = width // COLS
    packed = peers * PACK
    slots = peers * CAP
    place = jnp.asarray(unpack_matrix(), bf16)
    place_back = jnp.asarray(unpack_matrix().T, bf16)
    at = quarter.astype(jnp.int32)[None]

    pairs = (PAIR_A, PAIR_B)

    def swap(value, pairs):
        return lax.ppermute(value, "tp", pairs)

    def cut(value, at):
        return value[at]

    pairs = (PAIR_A, PAIR_B)
    half = width // 2
    gates = [
        [swap(expert_gate[0], PAIR_A)],
        [swap(expert_gate[1, i * half :][:half], PAIR_B) for i in range(2)],
    ]
    ups = [swap(cut(expert_up, e), pairs[e]) for e in range(2)]
    down_a = swap(expert_down, PAIR_A)
    down_b = swap(expert_down, PAIR_B)
    across = [swap(cut(down_b, 0), PAIR_A), swap(cut(down_a, 1), PAIR_B)]

    ranking = (pltpu.VMEM((peers, COLS * toks), f32), pltpu.VMEM((COLS * toks, part), bf16))
    message = jax.ShapeDtypeStruct((packed, part), bf16)
    h, send = call(
        norm_send_body,
        (jax.ShapeDtypeStruct((toks, width), bf16), message),
        ranking,
        count=4,
        smem=(0,),
    )(at, moe_input, moe_gain[None, :], expert_ids.T)
    sends = (
        send,
        call(send_body, message, ranking, count=3, smem=(0,))(at, h, expert_ids.T),
    )

    def over_ep(value):
        value = value.reshape(peers, PACK, part)
        return lax.all_to_all(value, "ep", 0, 0, tiled=True).reshape(packed, part)

    ff = expert_gate.shape[2]
    unpacking = (pltpu.VMEM((slots, width), bf16),)

    def hidden_half(rows, e):
        return call(
            functools.partial(hidden_body, e),
            jax.ShapeDtypeStruct((slots, 2 * ff), bf16),
            (
                *unpacking,
                pltpu.VMEM((width, 4 * ff), bf16),
                pltpu.SemaphoreType.DMA((5,)),
            ),
            count=5 + len(gates[e]),
            hbm=tuple(range(2, 5 + len(gates[e]))),
        )(rows, place, expert_gate, expert_up, ups[e], *gates[e])

    back = []
    for e in range(2):
        own = over_ep(sends[e])
        other = swap(own, pairs[1 - e])
        mine = hidden_half(own, e)
        theirs = hidden_half(other, e)
        theirs = swap(theirs, pairs[1 - e])
        weights = (expert_down, down_a, down_b, across[0])
        if e == 1:
            weights = (expert_down, down_b, down_a, across[1])
        back.append(
            call(
                functools.partial(down_body, e),
                jax.ShapeDtypeStruct((packed, part), bf16),
                (
                    pltpu.VMEM((slots, width), bf16),
                    pltpu.VMEM((4 * ff, width), bf16),
                    pltpu.VMEM((slots, 4 * ff), bf16),
                    pltpu.SemaphoreType.DMA((8,)),
                ),
                count=7,
                hbm=(2, 3, 4, 5),
            )(mine, theirs, *weights, place_back)
        )

    near = [swap(w, PAIR_A) for w in (shared_gate, shared_up, shared_down)]
    visitors = swap(h, PAIR_B)
    shared_own, shared_other = call(
        shared_body,
        (
            jax.ShapeDtypeStruct((toks, width), f32),
            jax.ShapeDtypeStruct((toks, width), bf16),
        ),
        count=8,
    )(h, visitors, shared_gate, shared_up, shared_down, *near)
    shared_more = swap(shared_other, PAIR_B)

    halo = tail_before(mix_input, mix_gain)
    mix_output = mixer(mix_input, mix_gain, halo, pool_weight, pool_scale)

    returned = over_ep(back[0])
    acc, route = call(
        first_body,
        (jax.ShapeDtypeStruct((toks, width), f32), jax.ShapeDtypeStruct((2 * toks, slots), bf16)),
        unpacking,
        count=6,
        smem=(0,),
    )(at, expert_ids, route_score, shared_own, returned, place)
    returned = over_ep(back[1])
    moe_output = call(
        last_body, jax.ShapeDtypeStruct((toks, width), bf16), unpacking, count=5
    )(acc, shared_more, route, returned, place)
    return (mix_output, moe_output)


def solution(mesh):
    return jax.shard_map(
        layer,
        mesh=mesh,
        in_specs=(
            P(("ep", "tp"), None),
            P(),
            P(),
            P(),
            P(("ep", "tp"), None),
            P(),
            P("ep", None),
            P(("ep", "tp"), None),
            P("ep", None, "tp"),
            P("ep", None, "tp"),
            P("ep", "tp", None),
            P(None, "tp"),
            P(None, "tp"),
            P("tp", None),
        ),
        out_specs=(P(("ep", "tp"), None), P(("ep", "tp"), None)),
        check_vma=False,
    )
```

```python
import functools

import jax
import jax.numpy as jnp
import numpy as np
from jax import lax
from jax.experimental import pallas as pl
from jax.experimental.pallas import tpu as pltpu
from jax.sharding import PartitionSpec as P


WINDOWS = (2, 4, 8, 16)
RMS_EPS = 1e-06
ROUTED_SCALE = 2.5
CAP = 6
COLS = 4
PACK = CAP * COLS
BLOCK = 8
SEND_BLOCK = 16
LATE_ROWS = 11
PAIR_A = ((0, 1), (1, 0), (2, 3), (3, 2))
PAIR_B = ((1, 2), (2, 1), (3, 0), (0, 3))


f32 = jnp.float32
bf16 = jnp.bfloat16


def dot32(a, b):
    return jnp.dot(a, b, preferred_element_type=f32)


def call(body, out, scratch=(), count=0, smem=(), hbm=()):
    def spec(i):
        if i in hbm:
            return pl.BlockSpec(memory_space=pltpu.HBM)
        return pl.BlockSpec(memory_space=pltpu.SMEM if i in smem else pltpu.VMEM)

    return pl.pallas_call(
        body, out_shape=out, in_specs=[spec(i) for i in range(count)], scratch_shapes=list(scratch)
    )


def unpack_matrix():
    rows = BLOCK * PACK
    per = BLOCK * CAP
    place = np.zeros((rows, rows), np.float32)
    for i in range(rows):
        q, rest = divmod(i, per)
        j, s = divmod(rest, CAP)
        place[i, j * PACK + q * CAP + s] = 1.0
    return place


def norm_send_body(at_ref, x_ref, gain_ref, ids_ref, h_ref, m_ref, rank_ref, hcat_ref):
    h_ref[...] = rms_norm(x_ref[...], gain_ref[...])
    send_rows(0, at_ref, h_ref, ids_ref, m_ref, rank_ref, hcat_ref)


def send_body(at_ref, h_ref, ids_ref, m_ref, rank_ref, hcat_ref):
    send_rows(1, at_ref, h_ref, ids_ref, m_ref, rank_ref, hcat_ref)


def send_rows(e, at_ref, h_ref, ids_ref, m_ref, rank_ref, hcat_ref):
    toks, width = h_ref.shape
    part = width // COLS
    for q in range(COLS):
        hcat_ref[q * toks : (q + 1) * toks, :] = h_ref[:, q * part : (q + 1) * part]
    peers = rank_ref.shape[0]
    ids = ids_ref[:, pl.ds(pl.multiple_of(at_ref[0] * toks, toks), toks)]
    expert = 2 * lax.broadcasted_iota(jnp.int32, (peers, toks), 0) + e
    named = jnp.zeros((peers, toks), f32)
    for k in range(ids.shape[0]):
        named = named + (ids[k : k + 1, :] == expert).astype(f32)
    before = (
        lax.broadcasted_iota(jnp.int32, (toks, toks), 0)
        < lax.broadcasted_iota(jnp.int32, (toks, toks), 1)
    ).astype(f32).astype(bf16)
    rank = jnp.where(named > 0, dot32(named.astype(bf16), before), -1.0)
    for q in range(COLS):
        rank_ref[:, q * toks : (q + 1) * toks] = rank

    def block(b, _):
        ranks = rank_ref[pl.ds(pl.multiple_of(b * SEND_BLOCK, SEND_BLOCK), SEND_BLOCK), :]
        shape = (SEND_BLOCK, PACK, COLS * toks)
        r = lax.broadcasted_iota(jnp.int32, shape, 1)
        col = lax.broadcasted_iota(jnp.int32, shape, 2)
        q = sum((r >= CAP * i).astype(jnp.int32) for i in range(1, COLS))
        want = jnp.where(
            (col >= q * toks) & (col < (q + 1) * toks), (r - CAP * q).astype(f32), -2.0
        )
        pick = (jnp.broadcast_to(ranks[:, None, :], shape) == want).astype(f32)
        pick = pick.reshape(SEND_BLOCK * PACK, COLS * toks).astype(bf16)
        rows = SEND_BLOCK * PACK
        m_ref[pl.ds(pl.multiple_of(b * rows, rows), rows), :] = dot32(
            pick, hcat_ref[...]
        ).astype(bf16)
        return 0

    lax.fori_loop(0, peers // SEND_BLOCK, block, 0)


def fetch(sources, targets, sems):
    copies = [
        pltpu.make_async_copy(src, dst, sems.at[i])
        for i, (src, dst) in enumerate(zip(sources, targets))
    ]
    for copy in copies:
        copy.start()
    return copies


def plane(ref, e):
    return ref.at[e] if len(ref.shape) == 3 else ref


def unpack_into(x_ref, place_ref, rows_ref):
    rows = BLOCK * PACK
    per = BLOCK * CAP
    part = x_ref.shape[1]

    def block(b, _):
        got = dot32(
            place_ref[...], x_ref[pl.ds(pl.multiple_of(b * rows, rows), rows), :]
        ).astype(bf16)
        for q in range(COLS):
            rows_ref[
                pl.ds(pl.multiple_of(b * per, per), per), q * part : (q + 1) * part
            ] = got[q * per : (q + 1) * per, :]
        return 0

    lax.fori_loop(0, x_ref.shape[0] // rows, block, 0, unroll=4)


def hidden_body(e, x_ref, place_ref, ga, ua, ub, *refs):
    *gb, hid_ref, rows_ref, held_ref, sems = refs
    w = held_ref.shape[1] // 4
    tall = held_ref.shape[0] // len(gb)
    targets = [held_ref.at[:, i * w : (i + 1) * w] for i in (0, 1, 3)]
    targets += [held_ref.at[i * tall : (i + 1) * tall, 2 * w : 3 * w] for i in range(len(gb))]
    copies = fetch([plane(ref, e) for ref in (ga, ua, ub, *gb)], targets, sems)
    unpack_into(x_ref, place_ref, rows_ref)
    for i, group in enumerate((copies[:2], copies[2:])):
        for copy in group:
            copy.wait()
        gate = dot32(rows_ref[...], held_ref[:, 2 * i * w : (2 * i + 1) * w])
        up = dot32(rows_ref[...], held_ref[:, (2 * i + 1) * w : (2 * i + 2) * w])
        hid_ref[:, i * w : (i + 1) * w] = (gate / (1.0 + jnp.exp(-gate)) * up).astype(bf16)


def down_body(e, mine_ref, theirs_ref, place_ref, *refs):
    *pieces, out_ref, y_ref, held_ref, hid_ref, sems = refs
    w = mine_ref.shape[1] // 2
    cols = held_ref.shape[1] // 2
    sides = [slice(c * cols, (c + 1) * cols) for c in range(2)]
    pieces = [plane(ref, e) for ref in pieces]
    ends = [sum(ref.shape[0] for ref in pieces[:i]) for i in range(len(pieces) + 1)]
    copies = [
        fetch(
            [ref.at[:, side] for ref in pieces],
            [held_ref.at[i:j, side] for i, j in zip(ends, ends[1:])],
            sems.at[pl.ds(len(pieces) * c, len(pieces))],
        )
        for c, side in enumerate(sides)
    ]
    hid_ref[:, : 2 * w] = mine_ref[...]
    hid_ref[:, 2 * w :] = theirs_ref[...]
    for side, group in zip(sides, copies):
        for copy in group:
            copy.wait()
        y_ref[:, side] = dot32(hid_ref[...], held_ref[:, side]).astype(bf16)
    rows = BLOCK * PACK
    per = BLOCK * CAP
    part = out_ref.shape[1]

    def block(b, _):
        at = pl.ds(pl.multiple_of(b * per, per), per)
        stack = jnp.concatenate(
            [y_ref[at, q * part : (q + 1) * part] for q in range(COLS)], axis=0
        )
        out_ref[pl.ds(pl.multiple_of(b * rows, rows), rows), :] = dot32(
            place_ref[...], stack
        ).astype(bf16)
        return 0

    lax.fori_loop(0, y_ref.shape[0] // per, block, 0, unroll=4)


def route_matrix(e, ids, score, peers):
    toks = ids.shape[0]
    total = peers * CAP
    weight = score / jnp.sum(score, axis=1, keepdims=True) * ROUTED_SCALE
    expert = 2 * lax.broadcasted_iota(jnp.int32, (toks, peers), 1) + e
    named = jnp.zeros((toks, peers), f32)
    scaled = jnp.zeros((toks, peers), f32)
    for k in range(ids.shape[1]):
        hit = ids[:, k : k + 1] == expert
        named = named + hit.astype(f32)
        scaled = scaled + jnp.where(hit, weight[:, k : k + 1], 0.0)
    before = (
        lax.broadcasted_iota(jnp.int32, (toks, toks), 1)
        < lax.broadcasted_iota(jnp.int32, (toks, toks), 0)
    ).astype(f32).astype(bf16)
    rank = jnp.where(named > 0, dot32(before, named.astype(bf16)), -1.0).astype(bf16)
    at = lax.broadcasted_iota(jnp.int32, (peers, total), 1) - CAP * lax.broadcasted_iota(
        jnp.int32, (peers, total), 0
    )
    mine = (at >= 0) & (at < CAP)
    spread = mine.astype(f32).astype(bf16)
    slot = jnp.sum(jnp.where(mine, at, 0).astype(f32), axis=0, keepdims=True)
    here = dot32(rank, spread) == slot
    high = scaled.astype(bf16)
    low = (scaled - high.astype(f32)).astype(bf16)
    return [jnp.where(here, dot32(piece, spread), 0.0).astype(bf16) for piece in (high, low)]


def first_body(
    at_ref, ids_ref, score_ref, base_ref, r_ref, place_ref, acc_ref, route_ref, rows_ref
):
    unpack_into(r_ref, place_ref, rows_ref)
    score = score_ref[...]
    toks = score.shape[0]
    ids = ids_ref[pl.ds(pl.multiple_of(at_ref[0] * toks, toks), toks), :]
    peers = rows_ref.shape[0] // CAP
    acc = base_ref[...]
    for piece in route_matrix(0, ids, score, peers):
        acc = acc + dot32(piece, rows_ref[...])
    acc_ref[...] = acc
    route_ref[:toks, :], route_ref[toks:, :] = route_matrix(1, ids, score, peers)


def last_body(acc_ref, more_ref, route_ref, r_ref, place_ref, out_ref, rows_ref):
    unpack_into(r_ref, place_ref, rows_ref)
    toks = acc_ref.shape[0]
    both = dot32(route_ref[...], rows_ref[...])
    acc = acc_ref[...] + more_ref[...].astype(f32) + both[:toks] + both[toks:]
    out_ref[...] = acc.astype(bf16)


def shared_body(own_ref, other_ref, ga, ua, da, gb, ub, db, own_out_ref, other_out_ref):
    for h_ref, out_ref in ((other_ref, other_out_ref), (own_ref, own_out_ref)):
        h = h_ref[...]
        total = None
        for g_ref, u_ref, d_ref in ((ga, ua, da), (gb, ub, db)):
            gate = dot32(h, g_ref[...])
            up = dot32(h, u_ref[...])
            hidden = (gate / (1.0 + jnp.exp(-gate)) * up).astype(bf16)
            piece = dot32(hidden, d_ref[...])
            total = piece if total is None else total + piece
        out_ref[...] = total.astype(out_ref.dtype)


def rms_norm(values, gain_row):
    upcast = values.astype(f32)
    scaled = upcast * lax.rsqrt(jnp.mean(upcast * upcast, axis=-1, keepdims=True) + RMS_EPS)
    return (scaled * gain_row).astype(bf16)


def mixer_body(at_ref, x_ref, gain_ref, halo_ref, pool_ref, scale_ref, out_ref, rows_ref):
    lead = halo_ref.shape[0]
    rows, width = x_ref.shape
    group = width // len(WINDOWS)
    rows_ref[:lead, :] = halo_ref[...]
    rows_ref[lead:, :] = rms_norm(x_ref[...], gain_ref[...])
    ahead = lax.broadcasted_iota(jnp.int32, (rows, lead + rows), 0) + lead
    back = ahead - lax.broadcasted_iota(jnp.int32, (rows, lead + rows), 1)
    taken = at_ref[0] + 1 + lax.broadcasted_iota(jnp.int32, (rows, 1), 0)
    for g, span in enumerate(WINDOWS):
        cols = slice(g * group, (g + 1) * group)
        band = ((back >= 0) & (back < span)).astype(f32).astype(bf16)
        pooled = dot32(band, rows_ref[:, cols]) / jnp.minimum(taken, span).astype(f32)
        difference = (pooled - rows_ref[lead:, cols].astype(f32)).astype(bf16)
        out_ref[:, cols] = (dot32(difference, pool_ref[g]) * scale_ref[:, cols]).astype(bf16)


def tail_before(mix_input, mix_gain):
    lead = max(WINDOWS)
    length = lax.axis_size(("ep", "tp"))
    return lax.ppermute(
        rms_norm(mix_input[mix_input.shape[0] - lead :], mix_gain),
        ("ep", "tp"),
        [(i, i + 1) for i in range(length - 1)],
    )


def mixer(mix_input, mix_gain, before, pool_weight, pool_scale):
    rows, width = mix_input.shape
    lead = before.shape[0]
    offset = (lax.axis_index(("ep", "tp")) * rows).astype(jnp.int32)
    return call(
        mixer_body,
        jax.ShapeDtypeStruct((rows, width), bf16),
        (pltpu.VMEM((lead + rows, width), bf16),),
        smem=(0,),
        count=6,
    )(offset[None], mix_input, mix_gain[None, :], before, pool_weight, pool_scale[None, :])


def layer(
    mix_input,
    mix_gain,
    pool_weight,
    pool_scale,
    moe_input,
    moe_gain,
    expert_ids,
    route_score,
    expert_gate,
    expert_up,
    expert_down,
    shared_gate,
    shared_up,
    shared_down,
):
    toks, width = moe_input.shape
    peers = lax.axis_size("ep")
    quarter = lax.axis_index("tp")
    part = width // COLS
    packed = peers * PACK
    slots = peers * CAP
    place = jnp.asarray(unpack_matrix(), bf16)
    place_back = jnp.asarray(unpack_matrix().T, bf16)
    at = quarter.astype(jnp.int32)[None]

    pairs = (PAIR_A, PAIR_B)

    def swap(value, pairs):
        return lax.ppermute(value, "tp", pairs)

    def cut(value, at):
        return value[at]

    pairs = (PAIR_A, PAIR_B)
    half = width // 2
    gates = [
        [swap(expert_gate[0], PAIR_A)],
        [swap(expert_gate[1, i * half :][:half], PAIR_B) for i in range(2)],
    ]
    ups = [swap(cut(expert_up, e), pairs[e]) for e in range(2)]
    down_b = swap(expert_down, PAIR_B)
    down_a = [swap(cut(expert_down, 0), PAIR_A)]
    cross = [swap(cut(down_b, 0), PAIR_A)]
    ranking = (pltpu.VMEM((peers, COLS * toks), f32), pltpu.VMEM((COLS * toks, part), bf16))
    message = jax.ShapeDtypeStruct((packed, part), bf16)
    h, send = call(
        norm_send_body,
        (jax.ShapeDtypeStruct((toks, width), bf16), message),
        ranking,
        count=4,
        smem=(0,),
    )(at, moe_input, moe_gain[None, :], expert_ids.T)
    late_down, _ = lax.optimization_barrier((expert_down, h))
    early = LATE_ROWS * expert_down.shape[1] // 16
    for span in (slice(0, early), slice(early, None)):
        down_a.append(swap(cut(late_down, (1, span)), PAIR_A))
        cross.append(swap(down_a[-1], PAIR_B))

    sends = (
        send,
        call(send_body, message, ranking, count=3, smem=(0,))(at, h, expert_ids.T),
    )

    def over_ep(value):
        value = value.reshape(peers, PACK, part)
        return lax.all_to_all(value, "ep", 0, 0, tiled=True).reshape(packed, part)

    ff = expert_gate.shape[2]
    unpacking = (pltpu.VMEM((slots, width), bf16),)

    def hidden_half(rows, e):
        return call(
            functools.partial(hidden_body, e),
            jax.ShapeDtypeStruct((slots, 2 * ff), bf16),
            (
                *unpacking,
                pltpu.VMEM((width, 4 * ff), bf16),
                pltpu.SemaphoreType.DMA((5,)),
            ),
            count=5 + len(gates[e]),
            hbm=tuple(range(2, 5 + len(gates[e]))),
        )(rows, place, expert_gate, expert_up, ups[e], *gates[e])

    back = []
    for e in range(2):
        own = over_ep(sends[e])
        other = swap(own, pairs[1 - e])
        mine = hidden_half(own, e)
        theirs = hidden_half(other, e)
        theirs = swap(theirs, pairs[1 - e])
        weights = (expert_down, down_a[0], down_b, cross[0])
        if e == 1:
            weights = (expert_down, down_b, *down_a[1:], *cross[1:])
        back.append(
            call(
                functools.partial(down_body, e),
                jax.ShapeDtypeStruct((packed, part), bf16),
                (
                    pltpu.VMEM((slots, width), bf16),
                    pltpu.VMEM((4 * ff, width), bf16),
                    pltpu.VMEM((slots, 4 * ff), bf16),
                    pltpu.SemaphoreType.DMA((2 * len(weights),)),
                ),
                count=3 + len(weights),
                hbm=tuple(range(3, 3 + len(weights))),
            )(mine, theirs, place_back, *weights)
        )

    near = [swap(w, PAIR_A) for w in (shared_gate, shared_up, shared_down)]
    visitors = swap(h, PAIR_B)
    shared_own, shared_other = call(
        shared_body,
        (
            jax.ShapeDtypeStruct((toks, width), f32),
            jax.ShapeDtypeStruct((toks, width), bf16),
        ),
        count=8,
    )(h, visitors, shared_gate, shared_up, shared_down, *near)
    shared_more = swap(shared_other, PAIR_B)

    halo = tail_before(mix_input, mix_gain)
    mix_output = mixer(mix_input, mix_gain, halo, pool_weight, pool_scale)

    returned = over_ep(back[0])
    acc, route = call(
        first_body,
        (jax.ShapeDtypeStruct((toks, width), f32), jax.ShapeDtypeStruct((2 * toks, slots), bf16)),
        unpacking,
        count=6,
        smem=(0,),
    )(at, expert_ids, route_score, shared_own, returned, place)
    returned = over_ep(back[1])
    moe_output = call(
        last_body, jax.ShapeDtypeStruct((toks, width), bf16), unpacking, count=5
    )(acc, shared_more, route, returned, place)
    return (mix_output, moe_output)


def solution(mesh):
    return jax.shard_map(
        layer,
        mesh=mesh,
        in_specs=(
            P(("ep", "tp"), None),
            P(),
            P(),
            P(),
            P(("ep", "tp"), None),
            P(),
            P("ep", None),
            P(("ep", "tp"), None),
            P("ep", None, "tp"),
            P("ep", None, "tp"),
            P("ep", "tp", None),
            P(None, "tp"),
            P(None, "tp"),
            P("tp", None),
        ),
        out_specs=(P(("ep", "tp"), None), P(("ep", "tp"), None)),
        check_vma=False,
    )
```
